32 devices in a mesh: kv: 16 (over z, y, core), tp: 2 (over x).
Axes of the slice: x: 2, y: 2, z: 4, core: 2. Of those that a mesh axis runs over, the one named last changes fastest.
Arguments:
- hidden_rows: bfloat16 [6144, 2048], P('kv'), may hold values from -6 to 6
- proj_query: bfloat16 [2048, 2048], P(None, 'tp'), may hold values from -0.125 to 0.125
- proj_key: bfloat16 [2048, 256], P(None, 'tp'), may hold values from -0.125 to 0.125
- proj_value: bfloat16 [2048, 256], P(None, 'tp'), may hold values from -0.125 to 0.125
- proj_output: bfloat16 [2048, 2048], P('tp'), may hold values from -0.125 to 0.125
- head_scale: float32 [32], P('tp'), may hold values from 0.25 to 96
- hot_blocks: int32 [16], replicated, may hold values from 0 to 191, as said below
- chosen_blocks: int32 [96, 16], P('kv'), may hold values from 0 to 27, as said below
Outputs:
- layer_out: bfloat16 [6144, 2048], P('kv', 'tp')
The draws below stay inside these ranges and needn't reach their ends.
Inputs may be any that keep to these rules, and one draw needn't show every extreme that they name: `hot_blocks`: 16 different key-block numbers; no device's 12 key blocks hold more than 2 of them, and in every draw some device holds exactly 2. `chosen_blocks`: each row's 16 codes name different key blocks; among them are the key blocks that cover the positions of query block b; no code of 12 or more names a block on the query block's own device.
All inputs are finite; a program needn't handle non-finite values.
Results may differ from the reference program's by a relative error of at most 0.01.
The reference program's roundings to bfloat16 on the way count: a program that leaves them out, or rounds other values in their place, can miss the bound.
Values may be sent and summed in bfloat16 or wider, within the bound.
No kernel may reach another device: no remote copies, remote signals or barrier semaphores. Data moves between devices by JAX's collectives and lax.ppermute only.
A program may use at most 64 MiB of HBM per device.

```python
import math
import jax
import jax.numpy as jnp
from jax import lax

D = 2048
H = 32
HD = 64
KVH = 4
KB = 32
QB = 64
NSEL = 16
NHOT = 16
TOK_DEV = 384
SEQ = 6144
NQB = 96
NKB = 192
KB_DEV = 12
N_KV = 16
N_TP = 2


def make_hot(key):
    base = jax.random.fold_in(key, 7001)
    key_perm, key_block, key_step, key_order = jax.random.split(base, 4)
    owners = jax.random.permutation(key_perm, N_KV).astype(jnp.int32)
    leader = owners[0]
    opposite = (leader + N_KV // 2) % N_KV
    remaining = owners[1:]
    order = jnp.argsort((remaining == opposite).astype(jnp.int32), stable=True)
    others = remaining[order][:NHOT - 3]
    owner_list = jnp.concatenate([jnp.stack([leader, leader, opposite]), others])
    blocks = jax.random.randint(key_block, (NHOT,), 0, KB_DEV, dtype=jnp.int32)
    offset_step = jax.random.randint(key_step, (), 1, KB_DEV, dtype=jnp.int32)
    blocks = blocks.at[1].set((blocks[0] + offset_step) % KB_DEV)
    block_ids = owner_list * KB_DEV + blocks
    return block_ids[jax.random.permutation(key_order, NHOT)].astype(jnp.int32)


def draw_hot_blocks(key, part):
    return make_hot(key)


def draw_chosen_blocks(key, part):
    hot = make_hot(key)
    per_block = QB // KB
    count = KB_DEV + NHOT
    qblock = jnp.arange(NQB, dtype=jnp.int32)
    device = qblock // (TOK_DEV // QB)
    local_ids = device[:, None] * KB_DEV + jnp.arange(KB_DEV, dtype=jnp.int32)[None, :]
    candidates = jnp.concatenate([local_ids, jnp.broadcast_to(hot[None, :], (NQB, NHOT))], axis=1)
    noise = jax.random.randint(jax.random.fold_in(key, 7002), (NQB, count), 0, 1000, dtype=jnp.int32)
    first_own = qblock * per_block
    own_cover = (candidates >= first_own[:, None]) & (candidates < first_own[:, None] + per_block)
    earlier = candidates < first_own[:, None] + per_block
    duplicate = (jnp.arange(count, dtype=jnp.int32)[None, :] >= KB_DEV) & (candidates // KB_DEV == device[:, None])
    score = noise + 10000 * earlier.astype(jnp.int32) + 100000 * own_cover.astype(jnp.int32)
    score = score - 1000000 * duplicate.astype(jnp.int32)
    score = score * count + jnp.arange(count, dtype=jnp.int32)[None, :]
    _, picked = lax.top_k(score, NSEL)
    return picked.astype(jnp.int32)


def draw_head_scale(key, part):
    key_low = jax.random.fold_in(jax.random.fold_in(key, 7003), 1)
    return jnp.exp(jax.random.uniform(key_low, (H,), jnp.float32, math.log(0.5), math.log(4.0)))


def levels(own_key, shape, cuts, low, high):
    level, own = 1.0, jax.random.fold_in(own_key, 6)
    for axis_at, parts in cuts:
        heights = jnp.exp(jax.random.uniform(jax.random.fold_in(own, axis_at), (parts,), jnp.float32, low / len(cuts), high / len(cuts)))
        level = level * jnp.repeat(heights, shape[axis_at] // parts).reshape([-1 if axis == axis_at else 1 for axis in range(len(shape))])
    return level


def gaussian(own_key, extent, deviation, limit, pieces=(), held_as=jnp.bfloat16):
    array = jax.random.normal(own_key, extent, jnp.float32) * deviation
    if len(pieces) > 0:
        array = levels(own_key, extent, pieces, -0.22, 0.18) * array
    return jnp.clip(array, min=-limit, max=limit).astype(held_as)


def setup_inputs(seed: int = 0) -> dict:
    splits = jax.random.split(jax.random.key(seed), 9)
    return {
        "hidden_rows": gaussian(splits[0], (SEQ, D), 1.0, 6.0, ((0, 16),)),
        "proj_query": gaussian(splits[1], (D, H * HD), D ** -0.5, 0.125, ((1, 2),)),
        "proj_key": gaussian(splits[2], (D, KVH * HD), D ** -0.5, 0.125, ((1, 2),)),
        "proj_value": gaussian(splits[3], (D, KVH * HD), D ** -0.5, 0.125, ((1, 2),)),
        "proj_output": gaussian(splits[4], (H * HD, D), (H * HD) ** -0.5, 0.125, ((0, 2),)),
        "head_scale": draw_head_scale(jax.random.fold_in(splits[8], 71), 0),
        "hot_blocks": draw_hot_blocks(jax.random.fold_in(splits[8], 71), 0),
        "chosen_blocks": draw_chosen_blocks(jax.random.fold_in(splits[8], 71), 0),
    }


def reference(hidden_rows, proj_query, proj_key, proj_value, proj_output, head_scale, hot_blocks, chosen_blocks):
    group_size = H // KVH
    per_device = TOK_DEV // QB
    queries = jnp.dot(hidden_rows, proj_query, preferred_element_type=jnp.float32).astype(jnp.bfloat16)
    key_proj = jnp.dot(hidden_rows, proj_key, preferred_element_type=jnp.float32).astype(jnp.bfloat16)
    value_proj = jnp.dot(hidden_rows, proj_value, preferred_element_type=jnp.float32).astype(jnp.bfloat16)
    queries = queries.reshape(NQB, QB, KVH, group_size, HD)
    key_proj = key_proj.reshape(NKB, KB, KVH, HD)
    value_proj = value_proj.reshape(NKB, KB, KVH, HD)
    scale_grid = head_scale.reshape(KVH, group_size)

    def attend(block_index):
        codes = chosen_blocks[block_index]
        holder = (block_index // per_device).astype(jnp.int32)
        hot_index = jnp.clip(codes - KB_DEV, 0, NHOT - 1).astype(jnp.int32)
        picked = jnp.where(codes < KB_DEV, holder * KB_DEV + codes, hot_blocks[hot_index]).astype(jnp.int32)
        key_rows = key_proj[picked].reshape(NSEL * KB, KVH, HD).astype(jnp.float32)
        value_rows = value_proj[picked].reshape(NSEL * KB, KVH, HD).astype(jnp.float32)
        query_rows = queries[block_index].astype(jnp.float32)
        scores = jnp.einsum('qcgd,lcd->cgql', query_rows, key_rows) * (HD ** -0.5)
        scores = scores * scale_grid[:, :, None, None]
        query_pos = block_index * QB + jnp.arange(QB, dtype=jnp.int32)
        key_pos = (picked[:, None] * KB + jnp.arange(KB, dtype=jnp.int32)[None, :]).reshape(NSEL * KB)
        visible = key_pos[None, :] <= query_pos[:, None]
        scores = jnp.where(visible[None, None], scores, -jnp.inf)
        row_max = jnp.max(scores, axis=-1, keepdims=True)
        lifted = jnp.exp(scores - row_max)
        weights = lifted / jnp.sum(lifted, axis=-1, keepdims=True)
        weights = lax.optimization_barrier(weights.astype(jnp.bfloat16)).astype(jnp.float32)
        attended = jnp.einsum('cgql,lcd->qcgd', weights, value_rows)
        return attended.reshape(QB, H * HD).astype(jnp.bfloat16)

    heads_out = lax.map(attend, jnp.arange(NQB, dtype=jnp.int32)).reshape(NQB * QB, H * HD)
    width = H * HD // N_TP
    total = jnp.zeros((NQB * QB, D), jnp.float32)
    for group_index in range(N_TP):
        begin = group_index * width
        partial_value = jnp.dot(heads_out[:, begin:begin + width], proj_output[begin:begin + width],
                          preferred_element_type=jnp.float32)
        total = total + lax.optimization_barrier(partial_value.astype(jnp.bfloat16)).astype(jnp.float32)
    return total.astype(jnp.bfloat16)
```

```python
import functools

import jax
import jax.numpy as jnp
from jax import lax
from jax.experimental import pallas as pl
from jax.experimental.pallas import tpu as pltpu
from jax.sharding import PartitionSpec as P

HD = 64
KB = 32
QB = 64
NSEL = 16
NHOT = 16
HOT_MOST = 2


def exchange_steps(count):
    steps = []
    step = 2
    while step < count:
        steps.append(step)
        step *= 2
    if count > 1:
        steps.append(1)
    return steps


def slot_kernel(hot, hidden, wk, wv, slots, table, rows, sem, *, own_blocks, steps):
    me = lax.axis_index("kv")
    owners = [lax.div(hot[h], own_blocks) for h in range(NHOT)]
    offs = [jnp.int32(0), jnp.int32(0)]
    ranks = []
    for h in range(NHOT):
        rank = jnp.int32(0)
        for g in range(h):
            rank = rank + jnp.where(owners[g] == owners[h], 1, 0)
        ranks.append(rank)
        mine = owners[h] == me
        for r in range(HOT_MOST):
            offs[r] = jnp.where(mine & (rank == r), hot[h] - owners[h] * own_blocks, offs[r])
    copies = []
    for r in range(HOT_MOST):
        copy = pltpu.make_async_copy(
            hidden.at[pl.ds(pl.multiple_of(offs[r] * KB, KB), KB)],
            rows.at[pl.ds(r * KB, KB)],
            sem.at[r],
        )
        copy.start()
        copies.append(copy)
    for h in range(NHOT):
        apart = owners[h] ^ me
        place = jnp.int32(0)
        for j, step in enumerate(steps):
            place = place + jnp.where((apart & step) != 0, 1 << j, 0)
        table[h] = (own_blocks + place * HOT_MOST + ranks[h]) * KB
    for copy in copies:
        copy.wait()
    x = rows[...]
    half = wk.shape[1]
    slots[:, :half] = jnp.dot(x, wk[...], preferred_element_type=jnp.float32).astype(jnp.bfloat16)
    slots[:, half:] = jnp.dot(x, wv[...], preferred_element_type=jnp.float32).astype(jnp.bfloat16)


def attend_kernel(
    codes,
    hot,
    table,
    scale,
    q,
    keys,
    values,
    near,
    far,
    wo,
    att,
    *rest,
    first,
    count,
    n_tp,
):
    *sends, pool, picked, s_buf, p_buf, wo_buf, sem = rest
    me = lax.axis_index("kv")
    here = lax.axis_index("tp")
    part = wo_buf.shape[2]
    loads = []
    for d in range(1, n_tp):
        there = lax.rem(here + d, n_tp)
        load = pltpu.make_async_copy(
            wo.at[:, pl.ds(pl.multiple_of(there * part, part), part)],
            wo_buf.at[d - 1],
            sem.at[d - 1],
        )
        load.start()
        loads.append(load)
    tok_rows, kw = keys.shape
    own_blocks = tok_rows // KB
    kv_heads = kw // HD
    group = q.shape[1] // HD // kv_heads
    near_rows = near.shape[0]
    pool[:tok_rows, :kw] = keys[...]
    pool[:tok_rows, kw:] = values[...]
    pool[tok_rows : tok_rows + near_rows, :] = near[...]
    pool[tok_rows + near_rows :, :] = far[...]
    lane = lax.broadcasted_iota(jnp.int32, (1, NSEL * KB), 1)
    lane_block = lane // KB
    for b in range(count):
        key_pos = lane - lane_block * KB
        for e in range(NSEL):
            code = codes[first + b, e]
            hot_at = jnp.maximum(code - own_blocks, 0)
            is_own = code < own_blocks
            row = jnp.where(is_own, code * KB, table[hot_at])
            block = jnp.where(is_own, me * own_blocks + code, hot[hot_at])
            key_pos = key_pos + jnp.where(lane_block == e, block * KB, 0)
            picked[e * KB : (e + 1) * KB, :] = pool[pl.ds(pl.multiple_of(row, KB), KB), :]
        query_pos = (
            me * tok_rows + (first + b) * QB + lax.broadcasted_iota(jnp.int32, (QB, 1), 0)
        )
        bias = jnp.where(key_pos <= query_pos, 0.0, -jnp.inf).astype(jnp.float32)
        for c in range(kv_heads):
            heads = [c * group + g for g in range(group)]
            q_rows = jnp.concatenate(
                [q[b * QB : (b + 1) * QB, h * HD : (h + 1) * HD] for h in heads], axis=0
            )
            s_buf[...] = lax.dot_general(
                q_rows,
                picked[:, c * HD : (c + 1) * HD],
                (((1,), (1,)), ((), ())),
                preferred_element_type=jnp.float32,
            )
            sums = []
            for g, h in enumerate(heads):
                at = slice(g * QB, (g + 1) * QB)
                s = s_buf[at, :] * (scale[h] * HD ** (-0.5)) + bias
                lifted = jnp.exp(s - jnp.max(s, axis=-1, keepdims=True))
                sums.append(jnp.sum(lifted, axis=-1, keepdims=True))
                p_buf[at, :] = lifted.astype(jnp.bfloat16)
            out = jnp.dot(
                p_buf[...],
                picked[:, kw + c * HD : kw + (c + 1) * HD],
                preferred_element_type=jnp.float32,
            )
            for g, h in enumerate(heads):
                att[b * QB : (b + 1) * QB, h * HD : (h + 1) * HD] = (
                    out[g * QB : (g + 1) * QB, :] / sums[g]
                ).astype(jnp.bfloat16)
    for d, send in enumerate(sends):
        loads[d].wait()
        send[...] = jnp.dot(att[...], wo_buf[d], preferred_element_type=jnp.float32).astype(
            jnp.bfloat16
        )


def own_kernel(*refs):
    *atts, wo, out, wo_buf, sem = refs
    half = wo_buf.shape[1]
    here = lax.axis_index("tp")
    load = pltpu.make_async_copy(
        wo.at[:, pl.ds(pl.multiple_of(here * half, half), half)], wo_buf, sem
    )
    load.start()
    load.wait()
    at = 0
    for a in atts:
        rows = a.shape[0]
        out[at : at + rows, :] = jnp.dot(
            a[...], wo_buf[...], preferred_element_type=jnp.float32
        ).astype(jnp.bfloat16)
        at += rows


def local(
    hidden_rows,
    proj_query,
    proj_key,
    proj_value,
    proj_output,
    head_scale,
    hot_blocks,
    chosen_blocks,
    *,
    n_kv,
    n_tp,
):
    tok_rows = hidden_rows.shape[0]
    own_blocks = tok_rows // KB
    kw = proj_key.shape[1]
    width = 2 * kw
    heads_w = proj_query.shape[1]
    part = proj_output.shape[1] // n_tp
    query_blocks = tok_rows // QB
    steps = exchange_steps(n_kv)
    smem = pl.BlockSpec(memory_space=pltpu.SMEM)
    vmem = pl.BlockSpec(memory_space=pltpu.VMEM)
    anym = pl.BlockSpec(memory_space=pl.ANY)
    slot_rows = HOT_MOST * KB
    slots, table = pl.pallas_call(
        functools.partial(slot_kernel, own_blocks=own_blocks, steps=steps),
        out_shape=(
            jax.ShapeDtypeStruct((slot_rows, width), jnp.bfloat16),
            jax.ShapeDtypeStruct((NHOT,), jnp.int32),
        ),
        in_specs=[smem, anym, vmem, vmem],
        out_specs=(vmem, smem),
        scratch_shapes=[
            pltpu.VMEM((slot_rows, hidden_rows.shape[1]), jnp.bfloat16),
            pltpu.SemaphoreType.DMA((HOT_MOST,)),
        ],
        name="slot_rows",
    )(hot_blocks, hidden_rows, proj_key, proj_value)

    def swap(x, step):
        return lax.ppermute(x, "kv", [(i, i ^ step) for i in range(n_kv)])

    near = slots
    for step in steps[:-1]:
        near = jnp.concatenate([near, swap(near, step)], axis=0)
    far = swap(near, steps[-1])

    def project(w):
        return jnp.dot(hidden_rows, w, preferred_element_type=jnp.float32).astype(jnp.bfloat16)

    queries = project(proj_query)
    keys = project(proj_key)
    values = project(proj_value)
    sizes = [1, 1] + [2] * ((query_blocks - 2) // 2)
    first = 0
    atts = []
    received = [[] for _ in range(1, n_tp)]
    group_rows = heads_w // HD // (kw // HD) * QB
    for count in sizes:
        rows = count * QB
        att, *sends = pl.pallas_call(
            functools.partial(attend_kernel, first=first, count=count, n_tp=n_tp),
            out_shape=[jax.ShapeDtypeStruct((rows, heads_w), jnp.bfloat16)]
            + [jax.ShapeDtypeStruct((rows, part), jnp.bfloat16)] * (n_tp - 1),
            in_specs=[smem, smem, smem, smem, vmem, vmem, vmem, vmem, vmem, anym],
            out_specs=[vmem] * n_tp,
            scratch_shapes=[
                pltpu.VMEM((tok_rows + near.shape[0] + far.shape[0], width), jnp.bfloat16),
                pltpu.VMEM((NSEL * KB, width), jnp.bfloat16),
                pltpu.VMEM((group_rows, NSEL * KB), jnp.float32),
                pltpu.VMEM((group_rows, NSEL * KB), jnp.bfloat16),
                pltpu.VMEM((n_tp - 1, proj_output.shape[0], part), jnp.bfloat16),
                pltpu.SemaphoreType.DMA((n_tp - 1,)),
            ],
            name="attend",
        )(
            chosen_blocks,
            hot_blocks,
            table,
            head_scale,
            queries[first * QB : first * QB + rows],
            keys,
            values,
            near,
            far,
            proj_output,
        )
        atts.append(att)
        for d, send in enumerate(sends):
            pairs = [(i, (i + d + 1) % n_tp) for i in range(n_tp)]
            received[d].append(lax.ppermute(send, "tp", pairs))
        first += count
    own = pl.pallas_call(
        own_kernel,
        out_shape=jax.ShapeDtypeStruct((tok_rows, part), jnp.bfloat16),
        in_specs=[vmem] * len(atts) + [anym],
        out_specs=vmem,
        scratch_shapes=[
            pltpu.VMEM((proj_output.shape[0], part), jnp.bfloat16),
            pltpu.SemaphoreType.DMA,
        ],
        name="own_part",
    )(*atts, proj_output)
    total = own.astype(jnp.float32)
    for pieces in received:
        total = total + jnp.concatenate(pieces, axis=0).astype(jnp.float32)
    return total.astype(jnp.bfloat16)


def solution(mesh):
    return jax.shard_map(
        functools.partial(local, n_kv=mesh.shape["kv"], n_tp=mesh.shape["tp"]),
        mesh=mesh,
        in_specs=(
            P("kv", None),
            P(None, "tp"),
            P(None, "tp"),
            P(None, "tp"),
            P("tp", None),
            P("tp"),
            P(),
            P("kv", None),
        ),
        out_specs=P("kv", "tp"),
        check_vma=False,
    )
```

```python
import functools

import jax
import jax.numpy as jnp
from jax import lax
from jax.experimental import pallas as pl
from jax.experimental.pallas import tpu as pltpu
from jax.sharding import PartitionSpec as P

HD = 64
KB = 32
QB = 64
NSEL = 16
NHOT = 16
HOT_MOST = 2


def exchange_steps(count):
    steps = []
    step = 2
    while step < count:
        steps.append(step)
        step *= 2
    if count > 1:
        steps.append(1)
    return steps


def slot_kernel(hot, hidden, wk, wv, slots, rows, sem, *, own_blocks):
    base = lax.axis_index("kv") * own_blocks
    offs = [jnp.int32(0) for _ in range(HOT_MOST)]
    seen = jnp.int32(0)
    for h in range(NHOT):
        off = hot[h] - base
        mine = (off >= 0) & (off < own_blocks)
        for r in range(HOT_MOST):
            offs[r] = jnp.where(mine & (seen == r), off, offs[r])
        seen = seen + jnp.where(mine, 1, 0)
    copies = []
    for r in range(HOT_MOST):
        copy = pltpu.make_async_copy(
            hidden.at[pl.ds(pl.multiple_of(offs[r] * KB, KB), KB)],
            rows.at[pl.ds(r * KB, KB)],
            sem.at[r],
        )
        copy.start()
        copies.append(copy)
    for copy in copies:
        copy.wait()
    x = rows[...]
    half = wk.shape[1]
    slots[:, :half] = jnp.dot(x, wk[...], preferred_element_type=jnp.float32).astype(jnp.bfloat16)
    slots[:, half:] = jnp.dot(x, wv[...], preferred_element_type=jnp.float32).astype(jnp.bfloat16)


def table_kernel(hot, table, *, own_blocks, steps):
    me = lax.axis_index("kv")
    owners = [lax.div(hot[h], own_blocks) for h in range(NHOT)]
    for h in range(NHOT):
        rank = jnp.int32(0)
        for g in range(h):
            rank = rank + jnp.where(owners[g] == owners[h], 1, 0)
        apart = owners[h] ^ me
        place = jnp.int32(0)
        for j, step in enumerate(steps):
            place = place + jnp.where((apart & step) != 0, 1 << j, 0)
        table[h] = (own_blocks + place * HOT_MOST + rank) * KB


def attend_kernel(
    codes,
    hot,
    table,
    scale,
    q,
    keys,
    values,
    near,
    far,
    *rest,
    first,
    count,
):
    att, pool, picked, s_buf, p_buf = rest[-5:]
    me = lax.axis_index("kv")
    tok_rows, kw = keys.shape
    own_blocks = tok_rows // KB
    kv_heads = kw // HD
    group = q.shape[1] // HD // kv_heads
    near_rows = near.shape[0]
    pool[:tok_rows, :kw] = keys[...]
    pool[:tok_rows, kw:] = values[...]
    pool[tok_rows : tok_rows + near_rows, :] = near[...]
    pool[tok_rows + near_rows :, :] = far[...]
    lane = lax.broadcasted_iota(jnp.int32, (1, NSEL * KB), 1)
    lane_block = lane // KB
    for b in range(count):
        key_pos = lane - lane_block * KB
        for e in range(NSEL):
            code = codes[first + b, e]
            hot_at = jnp.maximum(code - own_blocks, 0)
            is_own = code < own_blocks
            row = jnp.where(is_own, code * KB, table[hot_at])
            block = jnp.where(is_own, me * own_blocks + code, hot[hot_at])
            key_pos = key_pos + jnp.where(lane_block == e, block * KB, 0)
            picked[e * KB : (e + 1) * KB, :] = pool[pl.ds(pl.multiple_of(row, KB), KB), :]
        query_pos = (
            me * tok_rows + (first + b) * QB + lax.broadcasted_iota(jnp.int32, (QB, 1), 0)
        )
        bias = jnp.where(key_pos <= query_pos, 0.0, -jnp.inf).astype(jnp.float32)
        for c in range(kv_heads):
            heads = [c * group + g for g in range(group)]
            q_rows = jnp.concatenate(
                [q[b * QB : (b + 1) * QB, h * HD : (h + 1) * HD] for h in heads], axis=0
            )
            s_buf[...] = lax.dot_general(
                q_rows,
                picked[:, c * HD : (c + 1) * HD],
                (((1,), (1,)), ((), ())),
                preferred_element_type=jnp.float32,
            )
            sums = []
            for g, h in enumerate(heads):
                at = slice(g * QB, (g + 1) * QB)
                s = s_buf[at, :] * (scale[h] * HD ** (-0.5)) + bias
                lifted = jnp.exp(s - jnp.max(s, axis=-1, keepdims=True))
                sums.append(jnp.sum(lifted, axis=-1, keepdims=True))
                p_buf[at, :] = lifted.astype(jnp.bfloat16)
            out = jnp.dot(
                p_buf[...],
                picked[:, kw + c * HD : kw + (c + 1) * HD],
                preferred_element_type=jnp.float32,
            )
            for g, h in enumerate(heads):
                att[b * QB : (b + 1) * QB, h * HD : (h + 1) * HD] = (
                    out[g * QB : (g + 1) * QB, :] / sums[g]
                ).astype(jnp.bfloat16)


def local(
    hidden_rows,
    proj_query,
    proj_key,
    proj_value,
    proj_output,
    head_scale,
    hot_blocks,
    chosen_blocks,
    *,
    n_kv,
    n_tp,
):
    tok_rows = hidden_rows.shape[0]
    own_blocks = tok_rows // KB
    kw = proj_key.shape[1]
    width = 2 * kw
    heads_w = proj_query.shape[1]
    part = proj_output.shape[1] // n_tp
    query_blocks = tok_rows // QB
    steps = exchange_steps(n_kv)
    smem = pl.BlockSpec(memory_space=pltpu.SMEM)
    vmem = pl.BlockSpec(memory_space=pltpu.VMEM)
    anym = pl.BlockSpec(memory_space=pl.ANY)
    slot_rows = HOT_MOST * KB
    slots = pl.pallas_call(
        functools.partial(slot_kernel, own_blocks=own_blocks),
        out_shape=jax.ShapeDtypeStruct((slot_rows, width), jnp.bfloat16),
        in_specs=[smem, anym, vmem, vmem],
        out_specs=vmem,
        scratch_shapes=[
            pltpu.VMEM((slot_rows, hidden_rows.shape[1]), jnp.bfloat16),
            pltpu.SemaphoreType.DMA((HOT_MOST,)),
        ],
        name="slot_rows",
    )(hot_blocks, hidden_rows, proj_key, proj_value)
    table = pl.pallas_call(
        functools.partial(table_kernel, own_blocks=own_blocks, steps=steps),
        out_shape=jax.ShapeDtypeStruct((NHOT,), jnp.int32),
        in_specs=[smem],
        out_specs=smem,
        name="table",
    )(hot_blocks)

    def swap(x, step):
        return lax.ppermute(x, "kv", [(i, i ^ step) for i in range(n_kv)])

    def project(w):
        return jnp.dot(hidden_rows, w, preferred_element_type=jnp.float32).astype(jnp.bfloat16)

    here = lax.axis_index("tp")
    wo_parts = [
        lax.dynamic_slice_in_dim(proj_output, lax.rem(here + d, n_tp) * part, part, axis=1)
        for d in range(n_tp)
    ]
    queries = project(proj_query)
    keys = project(proj_key)
    values = project(proj_value)
    near = slots
    for step in steps[:-1]:
        near = jnp.concatenate([near, swap(near, step)], axis=0)
    near, table, keys, values, queries, *wo_parts = lax.optimization_barrier(
        (near, table, keys, values, queries, *wo_parts)
    )
    far = swap(near, steps[-1])
    per = 2 if query_blocks % 2 == 0 else 1
    rows = per * QB
    atts, pieces, sent = [], [], []
    group_rows = heads_w // HD // (kw // HD) * QB
    for chunk in range(query_blocks // per):
        att = pl.pallas_call(
            functools.partial(attend_kernel, first=chunk * per, count=per),
            out_shape=jax.ShapeDtypeStruct((rows, heads_w), jnp.bfloat16),
            grid=(1,),
            in_specs=[
                smem,
                smem,
                smem,
                smem,
                pl.BlockSpec((rows, heads_w), lambda i, chunk=chunk: (chunk, 0)),
                vmem,
                vmem,
                vmem,
                vmem,
            ]
            + [anym] * len(sent),
            out_specs=pl.BlockSpec((rows, heads_w), lambda i: (0, 0)),
            scratch_shapes=[
                pltpu.VMEM((tok_rows + near.shape[0] + far.shape[0], width), jnp.bfloat16),
                pltpu.VMEM((NSEL * KB, width), jnp.bfloat16),
                pltpu.VMEM((group_rows, NSEL * KB), jnp.float32),
                pltpu.VMEM((group_rows, NSEL * KB), jnp.bfloat16),
            ],
            name="attend",
        )(chosen_blocks, hot_blocks, table, head_scale, queries, keys, values, near, far, *sent)
        atts.append(att)
        got, sends = [], []
        for d in range(1, n_tp):
            send = jnp.dot(att, wo_parts[d], preferred_element_type=jnp.float32).astype(
                jnp.bfloat16
            )
            pairs = [(i, (i + d) % n_tp) for i in range(n_tp)]
            got.append(lax.ppermute(send, "tp", pairs))
            sends.append(send)
        sent = sends
        pieces.append(got)

    def total(own, got):
        out = own.astype(jnp.float32)
        for piece in got:
            out = out + piece.astype(jnp.float32)
        return out.astype(jnp.bfloat16)

    own = [
        jnp.dot(att, wo_parts[0], preferred_element_type=jnp.float32).astype(jnp.bfloat16)
        for att in atts
    ]
    sums = [total(o, g) for o, g in zip(own[:-1], pieces[:-1])]
    out = jnp.concatenate(sums + [own[-1]], axis=0)
    out, last = lax.optimization_barrier((out, own[-1]))
    return lax.dynamic_update_slice(out, total(last, pieces[-1]), (tok_rows - rows, 0))


def solution(mesh):
    return jax.shard_map(
        functools.partial(local, n_kv=mesh.shape["kv"], n_tp=mesh.shape["tp"]),
        mesh=mesh,
        in_specs=(
            P("kv", None),
            P(None, "tp"),
            P(None, "tp"),
            P(None, "tp"),
            P("tp", None),
            P("tp"),
            P(),
            P("kv", None),
        ),
        out_specs=P("kv", "tp"),
        check_vma=False,
    )
```

```python
import functools

import jax
import jax.numpy as jnp
from jax import lax
from jax.experimental import pallas as pl
from jax.experimental.pallas import tpu as pltpu
from jax.sharding import PartitionSpec as P


HD = 64
KB = 32
QB = 64
NSEL = 16
NHOT = 16
HOT_MOST = 2


def exchange_steps(count):
    steps = []
    step = 2
    while step < count:
        steps.append(step)
        step *= 2
    if count > 1:
        steps.append(1)
    return steps


def slot_kernel(hot, hidden, wk, wv, slots, rows, sem, *, own_blocks):
    base = lax.axis_index("kv") * own_blocks
    offs = [jnp.int32(0) for _ in range(HOT_MOST)]
    seen = jnp.int32(0)
    for h in range(NHOT):
        off = hot[h] - base
        mine = (off >= 0) & (off < own_blocks)
        for r in range(HOT_MOST):
            offs[r] = jnp.where(mine & (seen == r), off, offs[r])
        seen = seen + jnp.where(mine, 1, 0)
    copies = []
    for r in range(HOT_MOST):
        copy = pltpu.make_async_copy(
            hidden.at[pl.ds(pl.multiple_of(offs[r] * KB, KB), KB)],
            rows.at[pl.ds(r * KB, KB)],
            sem.at[r],
        )
        copy.start()
        copies.append(copy)
    for copy in copies:
        copy.wait()
    x = rows[...]
    half = wk.shape[1]
    slots[:, :half] = jnp.dot(x, wk[...], preferred_element_type=jnp.float32).astype(jnp.bfloat16)
    slots[:, half:] = jnp.dot(x, wv[...], preferred_element_type=jnp.float32).astype(jnp.bfloat16)


def table_kernel(hot, table, *, own_blocks, steps):
    me = lax.axis_index("kv")
    owners = [lax.div(hot[h], own_blocks) for h in range(NHOT)]
    for h in range(NHOT):
        rank = jnp.int32(0)
        for g in range(h):
            rank = rank + jnp.where(owners[g] == owners[h], 1, 0)
        apart = owners[h] ^ me
        place = jnp.int32(0)
        for j, step in enumerate(steps):
            place = place + jnp.where((apart & step) != 0, 1 << j, 0)
        table[h] = (own_blocks + place * HOT_MOST + rank) * KB


def attend_kernel(
    codes,
    hot,
    table,
    scale,
    q,
    keys,
    values,
    near,
    far,
    *rest,
    first,
    count,
):
    att, pool, picked, s_buf, p_buf = rest[-5:]
    me = lax.axis_index("kv")
    tok_rows, kw = keys.shape
    own_blocks = tok_rows // KB
    kv_heads = kw // HD
    group = q.shape[1] // HD // kv_heads
    near_rows = near.shape[0]
    pool[:tok_rows, :kw] = keys[...]
    pool[:tok_rows, kw:] = values[...]
    pool[tok_rows : tok_rows + near_rows, :] = near[...]
    pool[tok_rows + near_rows :, :] = far[...]
    lane = lax.broadcasted_iota(jnp.int32, (1, NSEL * KB), 1)
    lane_block = lane // KB
    for b in range(count):
        key_pos = lane - lane_block * KB
        for e in range(NSEL):
            code = codes[first + b, e]
            hot_at = jnp.maximum(code - own_blocks, 0)
            is_own = code < own_blocks
            row = jnp.where(is_own, code * KB, table[hot_at])
            block = jnp.where(is_own, me * own_blocks + code, hot[hot_at])
            key_pos = key_pos + jnp.where(lane_block == e, block * KB, 0)
            picked[e * KB : (e + 1) * KB, :] = pool[pl.ds(pl.multiple_of(row, KB), KB), :]
        query_pos = (
            me * tok_rows + (first + b) * QB + lax.broadcasted_iota(jnp.int32, (QB, 1), 0)
        )
        bias = jnp.where(key_pos <= query_pos, 0.0, -jnp.inf).astype(jnp.float32)
        for c in range(kv_heads):
            heads = [c * group + g for g in range(group)]
            q_rows = jnp.concatenate(
                [q[b * QB : (b + 1) * QB, h * HD : (h + 1) * HD] for h in heads], axis=0
            )
            s_buf[...] = lax.dot_general(
                q_rows,
                picked[:, c * HD : (c + 1) * HD],
                (((1,), (1,)), ((), ())),
                preferred_element_type=jnp.float32,
            )
            sums = []
            for g, h in enumerate(heads):
                at = slice(g * QB, (g + 1) * QB)
                s = s_buf[at, :] * (scale[h] * HD ** (-0.5)) + bias
                lifted = jnp.exp(s - jnp.max(s, axis=-1, keepdims=True))
                sums.append(jnp.sum(lifted, axis=-1, keepdims=True))
                p_buf[at, :] = lifted.astype(jnp.bfloat16)
            out = jnp.dot(
                p_buf[...],
                picked[:, kw + c * HD : kw + (c + 1) * HD],
                preferred_element_type=jnp.float32,
            )
            for g, h in enumerate(heads):
                att[b * QB : (b + 1) * QB, h * HD : (h + 1) * HD] = (
                    out[g * QB : (g + 1) * QB, :] / sums[g]
                ).astype(jnp.bfloat16)


def local(
    hidden_rows,
    proj_query,
    proj_key,
    proj_value,
    proj_output,
    head_scale,
    hot_blocks,
    chosen_blocks,
    *,
    n_kv,
    n_tp,
):
    tok_rows = hidden_rows.shape[0]
    own_blocks = tok_rows // KB
    kw = proj_key.shape[1]
    width = 2 * kw
    heads_w = proj_query.shape[1]
    part = proj_output.shape[1] // n_tp
    query_blocks = tok_rows // QB
    steps = exchange_steps(n_kv)
    smem = pl.BlockSpec(memory_space=pltpu.SMEM)
    vmem = pl.BlockSpec(memory_space=pltpu.VMEM)
    anym = pl.BlockSpec(memory_space=pl.ANY)
    slot_rows = HOT_MOST * KB
    slots = pl.pallas_call(
        functools.partial(slot_kernel, own_blocks=own_blocks),
        out_shape=jax.ShapeDtypeStruct((slot_rows, width), jnp.bfloat16),
        in_specs=[smem, anym, vmem, vmem],
        out_specs=vmem,
        scratch_shapes=[
            pltpu.VMEM((slot_rows, hidden_rows.shape[1]), jnp.bfloat16),
            pltpu.SemaphoreType.DMA((HOT_MOST,)),
        ],
        name="slot_rows",
    )(hot_blocks, hidden_rows, proj_key, proj_value)
    table = pl.pallas_call(
        functools.partial(table_kernel, own_blocks=own_blocks, steps=steps),
        out_shape=jax.ShapeDtypeStruct((NHOT,), jnp.int32),
        in_specs=[smem],
        out_specs=smem,
        name="table",
    )(hot_blocks)

    def swap(x, step):
        return lax.ppermute(x, "kv", [(i, i ^ step) for i in range(n_kv)])

    def project(w):
        return jnp.dot(hidden_rows, w, preferred_element_type=jnp.float32).astype(
            jnp.bfloat16
        )

    here = lax.axis_index("tp")

    def wo_cols(w, d):
        return lax.dynamic_slice_in_dim(w, lax.rem(here + d, n_tp) * part, part, axis=1)

    wo_parts = [wo_cols(proj_output, d) for d in range(1, n_tp)]
    queries = project(proj_query)
    keys = project(proj_key)
    values = project(proj_value)
    near = slots
    for step in steps[:-1]:
        near = jnp.concatenate([near, swap(near, step)], axis=0)
    near, table, keys, values, queries, *wo_parts = lax.optimization_barrier(
        (near, table, keys, values, queries, *wo_parts)
    )
    far = swap(near, steps[-1])
    per = 3 if query_blocks % 3 == 0 else 1
    rows = per * QB
    atts, pieces, sent = [], [], []
    group_rows = heads_w // HD // (kw // HD) * QB
    for chunk in range(query_blocks // per):
        att = pl.pallas_call(
            functools.partial(attend_kernel, first=chunk * per, count=per),
            out_shape=jax.ShapeDtypeStruct((rows, heads_w), jnp.bfloat16),
            grid=(1,),
            in_specs=[
                smem,
                smem,
                smem,
                smem,
                pl.BlockSpec((rows, heads_w), lambda i, chunk=chunk: (chunk, 0)),
                vmem,
                vmem,
                vmem,
                vmem,
            ]
            + [anym] * len(sent),
            out_specs=pl.BlockSpec((rows, heads_w), lambda i: (0, 0)),
            scratch_shapes=[
                pltpu.VMEM((tok_rows + near.shape[0] + far.shape[0], width), jnp.bfloat16),
                pltpu.VMEM((NSEL * KB, width), jnp.bfloat16),
                pltpu.VMEM((group_rows, NSEL * KB), jnp.float32),
                pltpu.VMEM((group_rows, NSEL * KB), jnp.bfloat16),
            ],
            name="attend",
        )(chosen_blocks, hot_blocks, table, head_scale, queries, keys, values, near, far, *sent)
        atts.append(att)
        got, sends = [], []
        for d in range(1, n_tp):
            send = jnp.dot(att, wo_parts[d - 1], preferred_element_type=jnp.float32).astype(
                jnp.bfloat16
            )
            pairs = [(i, (i + d) % n_tp) for i in range(n_tp)]
            got.append(lax.ppermute(send, "tp", pairs))
            sends.append(send)
        sent = sends
        pieces.append(got)

    def total(own, got):
        out = own.astype(jnp.float32)
        for piece in got:
            out = out + piece.astype(jnp.float32)
        return out.astype(jnp.bfloat16)

    wo_late, *atts = lax.optimization_barrier((proj_output, *atts))
    own_all = jnp.dot(
        jnp.concatenate(atts, axis=0), wo_cols(wo_late, 0), preferred_element_type=jnp.float32
    ).astype(jnp.bfloat16)
    own = [own_all[i * rows : (i + 1) * rows] for i in range(len(atts))]
    sums = [total(o, g) for o, g in zip(own[:-1], pieces[:-1])]
    out = jnp.concatenate(sums + [own[-1]], axis=0)
    out, last = lax.optimization_barrier((out, own[-1]))
    return lax.dynamic_update_slice(out, total(last, pieces[-1]), (tok_rows - rows, 0))


def solution(mesh):
    return jax.shard_map(
        functools.partial(local, n_kv=mesh.shape["kv"], n_tp=mesh.shape["tp"]),
        mesh=mesh,
        in_specs=(
            P("kv", None),
            P(None, "tp"),
            P(None, "tp"),
            P(None, "tp"),
            P("tp", None),
            P("tp"),
            P(),
            P("kv", None),
        ),
        out_specs=P("kv", "tp"),
        check_vma=False,
    )
```
